32 devices in a mesh: ep: 8 (over z, core), tp: 4 (over y, x).
Axes of the slice: x: 2, y: 2, z: 4, core: 2. Of those that a mesh axis runs over, the one named last changes fastest.
Arguments:
- tokens: bfloat16 [1024, 4096], P('ep', 'tp'), may hold values from -6 to 6
- out_grad: bfloat16 [1024, 4096], P('ep', 'tp'), may hold values from -1.5 to 1.5
- routes: int32 [1024, 2], P('ep'), may hold values from 0 to 7, all different within a row; in each aligned block of 128 rows (0 to 127, 128 to 255, ...) at most 40 rows name the same one
- route_weights: float32 [1024, 2], P('ep'), may hold values from 0.2 to 1.2
- gate_proj: bfloat16 [8, 1024, 4096], P('ep', 'tp'), may hold values from -0.09375 to 0.09375
- up_proj: bfloat16 [8, 1024, 4096], P('ep', 'tp'), may hold values from -0.09375 to 0.09375
- down_proj: bfloat16 [8, 1024, 4096], P('ep', 'tp'), may hold values from -0.1875 to 0.1875
- shared_hidden: bfloat16 [1024, 1024], P('ep'), may hold values from -6 to 6
Outputs:
- token_grad: bfloat16 [1024, 4096], P('ep', 'tp')
- weight_grad: float32 [1024, 2], P('ep')
- gate_grad: bfloat16 [8, 1024, 4096], P('ep', 'tp')
- up_grad: bfloat16 [8, 1024, 4096], P('ep', 'tp')
- down_grad: bfloat16 [8, 1024, 4096], P('ep', 'tp')
- shared_grad: float32 [1024, 4096], P('ep', 'tp')
The draws below stay inside these ranges and needn't reach their ends.
Inputs may be any that keep to these rules, and one draw needn't show every extreme that they name: Within each block of 128 consecutive tokens, no expert is named by more than 40 routes, and in some blocks one expert is named by exactly 40. The 2 experts of one token differ.
All inputs are finite; a program needn't handle non-finite values.
Results may differ from the reference program's by a relative error of at most 0.0065.
Values may be sent and summed in bfloat16 or wider, within the bound.
No kernel may reach another device: no remote copies, remote signals or barrier semaphores. Data moves between devices by JAX's collectives and lax.ppermute only.
A program may use at most 64 MiB of HBM per device.

```python
import math
import jax
import jax.numpy as jnp
import numpy as np
from jax import lax

D = 4096
FE = 1024
FS = 1024
TOP = 2
TOK_DEV = 128
EXPERTS = 8
TOKENS = 1024
CAP = 40
N_EP = 8
N_TP = 4


def strengthened(array, key, source, target, parts, factor):
    owner, partner = [(jnp.arange(array.shape[position]) // (array.shape[position] // parts)).reshape([-1 if axis == position else 1 for axis in range(array.ndim)]) for position in (source, target)]
    chosen = jax.random.permutation(key, parts)[partner]
    strong = (owner == chosen) | (owner == (partner + parts // 2) % parts)
    return jnp.where(strong, factor * array, array)


def steps_of(rng, extent, split, smallest, top_value):
    def one(axis_at, parts):
        steps = jax.random.uniform(jax.random.fold_in(jax.random.fold_in(rng, 6), axis_at), (parts,), jnp.float32, smallest / len(split), top_value / len(split))
        return jnp.repeat(jnp.exp(steps), extent[axis_at] // parts).reshape((-1,) + (1,) * (len(extent) - axis_at - 1))

    gain = one(*split[0])
    for cut in split[1:]:
        gain = gain * one(*cut)
    return gain


def shared_out(rng, own, number, rows, number_of, top, bound, slope):
    sequence = jax.random.permutation(rng, number_of)
    heavy_load, common = portions_of(number_of, rows * top, bound, slope, True), portions_of(number_of, rows * top, bound, slope, False)
    places = jnp.arange(number_of)

    def named(lengths, rotation):
        used = int((lengths > 0).sum())
        fixed = max(1, used // 4)
        moved = fixed + (places - fixed + rotation * (used - fixed)) % max(1, number_of - fixed)
        return jnp.zeros((number_of,), jnp.int32).at[sequence[jnp.where(places < fixed, places, moved)]].set(jnp.asarray(lengths, jnp.int32))

    lengths = jnp.where(number % 4 == 0, named(heavy_load, number // 4), named(common, number - number // 4 - 1))
    mixed = jax.random.permutation(jax.random.fold_in(own, 3), number_of)
    source_of, taker = mixed[0:number_of // 2 * 2:2], mixed[1:number_of // 2 * 2:2]
    room = jnp.minimum(lengths[source_of] - 1, bound - lengths[taker]) // 2
    room = jnp.where((source_of == sequence[0]) | (taker == sequence[0]) | (lengths[taker] == 0), 0, jnp.maximum(room, 0))
    moved = jax.random.randint(jax.random.fold_in(own, 4), (number_of // 2,), 0, 1 << 20) % (room + 1)
    lengths = lengths.at[source_of].add(-moved).at[taker].add(moved)
    members = jnp.searchsorted(jnp.cumsum(lengths), jnp.arange(rows * top), side="right").astype(jnp.int32)
    table = members.reshape(top, rows).T
    table = table[jax.random.permutation(jax.random.fold_in(own, 1), rows)]
    rotation = jax.random.randint(jax.random.fold_in(own, 2), (rows, 1), 0, top)
    return jnp.take_along_axis(table, (jnp.arange(top)[None, :] + rotation) % top, axis=1)


def portions_of(amount, total, bound, slope, full):
    loads = [(1 << 20) // math.isqrt(grade ** slope) + 1 for grade in range(1, amount + 1)]
    largest = bound if full else min(bound, max(-(-total // amount), total * loads[0] // sum(loads)))
    least = 1 if total - largest >= amount - 1 else 0
    holding, spare = [largest] + [least] * (amount - 1), total - largest - least * (amount - 1)
    while spare > 0:
        free = [i for i in range(1, amount) if holding[i] < largest] or [i for i in range(1, amount) if holding[i] < bound]
        mass, remaining = sum([loads[i] for i in free]), spare
        for i in free:
            addition = min(bound - holding[i], max(1, remaining * loads[i] // mass), spare)
            holding[i] = holding[i] + addition
            spare = spare - addition
    return np.array(holding)


def bell_draw(rng, extent, spread, bound, split=(), held_as=jnp.bfloat16):
    level = steps_of(rng, extent, split, -0.22, 0.18) if split else 1.0
    array = jax.random.normal(rng, extent, jnp.float32) * spread * level
    return jnp.minimum(jnp.maximum(array, -bound), bound).astype(held_as)


def gaussian_with(key, extent, scale, most, cuts, heavy, kind=jnp.bfloat16):
    result = scale * jax.random.normal(key, extent, jnp.float32)
    if cuts:
        result = result * steps_of(key, extent, cuts, -0.22, 0.18)
    return jnp.clip(strengthened(result, jax.random.fold_in(key, 3), *heavy), -most, most).astype(kind)


def setup_inputs(seed: int = 0) -> dict:
    streams_of = jax.random.split(jax.random.key(seed), 9)
    tokens = bell_draw(streams_of[0], (TOKENS, D), 1.0, 6.0, ((0, 8), (1, 4)))
    out_grad = bell_draw(streams_of[1], (TOKENS, D), 0.25, 1.5, ((0, 8), (1, 4)))
    routes_keys = jax.random.split(jax.random.fold_in(streams_of[2], 1), TOKENS // TOK_DEV)
    routes_turns = jax.random.permutation(jax.random.fold_in(streams_of[2], 3), TOKENS // TOK_DEV)
    routes = jax.vmap(lambda own, number: shared_out(jax.random.fold_in(streams_of[2], 2), own, number, TOK_DEV, EXPERTS, TOP, CAP, 2))(routes_keys, routes_turns).reshape((TOKENS, TOP))
    route_weights = jnp.clip(0.2 + 1 * jax.random.uniform(streams_of[3], (TOKENS, TOP), jnp.float32) ** steps_of(streams_of[3], (TOKENS, TOP), ((0, 8),), -0.2, 0.2), 0.2, 1.2)
    gate_proj = bell_draw(streams_of[4], (EXPERTS, FE, D), D ** -0.5, 0.09375, ((0, 8), (1, 4)))
    up_proj = bell_draw(streams_of[5], (EXPERTS, FE, D), D ** -0.5, 0.09375, ((0, 8), (1, 4)))
    down_proj = bell_draw(streams_of[6], (EXPERTS, FE, D), FE ** -0.5, 0.1875, ((0, 8), (1, 4)))
    shared_hidden = gaussian_with(streams_of[7], (TOKENS, FS), 1.0, 6.0, ((0, 8),), (0, 1, 8, 2.0))
    return {"tokens": tokens, "out_grad": out_grad, "routes": routes, "route_weights": route_weights, "gate_proj": gate_proj, "up_proj": up_proj, "down_proj": down_proj, "shared_hidden": shared_hidden}


def reference(tokens, out_grad, routes, route_weights, gate_proj, up_proj, down_proj, shared_hidden):
    block_routes = TOK_DEV * TOP
    expert_rows = N_EP * CAP
    flat_routes = routes.reshape(N_EP, block_routes)
    expert_ids = jnp.arange(EXPERTS, dtype=jnp.int32)
    onehot = (flat_routes[:, :, None] == expert_ids[None, None, :]).astype(jnp.int32)
    slot_rank = jnp.sum((jnp.cumsum(onehot, axis=1) - 1) * onehot, axis=2)
    block_ids = jnp.arange(N_EP, dtype=jnp.int32)[:, None]
    slot_index = (flat_routes * expert_rows + block_ids * CAP + slot_rank).reshape(-1).astype(jnp.int32)
    route_ids = jnp.arange(TOKENS * TOP, dtype=jnp.int32)
    route_of_slot = jnp.full((EXPERTS * expert_rows,), -1, jnp.int32).at[slot_index].set(route_ids)
    filled = route_of_slot >= 0
    safe_route = jnp.maximum(route_of_slot, 0).astype(jnp.int32)
    token_of_slot = (safe_route // TOP).astype(jnp.int32)
    weight_b = lax.optimization_barrier(route_weights.reshape(-1).astype(jnp.bfloat16)).astype(jnp.float32)
    slot_weight = jnp.where(filled, weight_b[safe_route], jnp.zeros((), jnp.float32))
    zero_value = jnp.zeros((), jnp.bfloat16)
    slot_tokens = jnp.where(filled[:, None], tokens[token_of_slot], zero_value).reshape(EXPERTS, expert_rows, D)
    slot_grads = jnp.where(filled[:, None], out_grad[token_of_slot], zero_value).reshape(EXPERTS, expert_rows, D)
    slot_scale = slot_weight.reshape(EXPERTS, expert_rows)
    block_width = FE // N_TP
    contract_features = (((1,), (1,)), ((), ()))
    contract_rows = (((0,), (0,)), ((), ()))

    def one_expert(operands):
        rows_in, grads_in, scale, gate_matrix, up_matrix, down_matrix = operands
        pre_gate = lax.dot_general(rows_in, gate_matrix, contract_features, preferred_element_type=jnp.float32)
        pre_up = lax.dot_general(rows_in, up_matrix, contract_features, preferred_element_type=jnp.float32)
        squash = jax.nn.sigmoid(pre_gate)
        activated = pre_gate * squash
        hidden = lax.optimization_barrier((activated * pre_up).astype(jnp.bfloat16))
        back_grad = lax.dot_general(grads_in, down_matrix, contract_features,
                                    preferred_element_type=jnp.float32)
        products = jnp.sum(hidden.astype(jnp.float32) * back_grad, axis=1)
        hidden_grad = scale[:, None] * back_grad
        scaled_hidden = (scale[:, None] * hidden.astype(jnp.float32)).astype(jnp.bfloat16)
        gate_delta = (hidden_grad * pre_up * squash * (1.0 + pre_gate * (1.0 - squash))).astype(jnp.bfloat16)
        up_delta = (hidden_grad * activated).astype(jnp.bfloat16)
        gate_part = lax.dot_general(gate_delta, rows_in, contract_rows,
                                    preferred_element_type=jnp.float32).astype(jnp.bfloat16)
        up_part = lax.dot_general(up_delta, rows_in, contract_rows,
                                  preferred_element_type=jnp.float32).astype(jnp.bfloat16)
        down_part = lax.dot_general(scaled_hidden, grads_in, contract_rows,
                                    preferred_element_type=jnp.float32).astype(jnp.bfloat16)
        gate_blocks = gate_delta.astype(jnp.float32).reshape(-1, N_TP, block_width)
        up_blocks = up_delta.astype(jnp.float32).reshape(-1, N_TP, block_width)
        gate_weights = gate_matrix.astype(jnp.float32).reshape(N_TP, block_width, D)
        up_weights = up_matrix.astype(jnp.float32).reshape(N_TP, block_width, D)
        block_part = jnp.einsum('rtf,tfd->trd', gate_blocks, gate_weights) + jnp.einsum('rtf,tfd->trd', up_blocks, up_weights)
        block_part = lax.optimization_barrier(block_part.astype(jnp.bfloat16)).astype(jnp.float32)
        return jnp.sum(block_part, axis=0), products, gate_part, up_part, down_part

    route_rows, products, gate_grad, up_grad, down_grad = lax.map(
        one_expert, (slot_tokens, slot_grads, slot_scale, gate_proj, up_proj, down_proj))
    route_rows = route_rows.reshape(EXPERTS * expert_rows, D)
    products = products.reshape(-1)
    token_grad = jnp.sum(route_rows[slot_index].reshape(TOKENS, TOP, D), axis=1).astype(jnp.bfloat16)
    weight_grad = products[slot_index].reshape(TOKENS, TOP)
    shared_grad = lax.dot_general(shared_hidden, out_grad, (((0,), (0,)), ((), ())),
                                  preferred_element_type=jnp.float32)
    return token_grad, weight_grad, gate_grad, up_grad, down_grad, shared_grad
```

```python
import functools

import jax
import jax.numpy as jnp
from jax import lax
from jax.experimental import pallas as pl
from jax.experimental.pallas import tpu as pltpu
from jax.sharding import PartitionSpec as P


CORES = 2
META = 8
LANES = 128
BF = jnp.bfloat16
F32 = jnp.float32
VMEM_LIMIT = 56 * 1024 * 1024


def xor_permute(value, axis, offset):
    size = lax.axis_size(axis)
    return lax.ppermute(value, axis, [(i, i ^ offset) for i in range(size)])


def nn(a, b):
    return lax.dot_general(a, b, (((1,), (0,)), ((), ())), preferred_element_type=F32)


def nt(a, b):
    return lax.dot_general(a, b, (((1,), (1,)), ((), ())), preferred_element_type=F32)


def tn(a, b):
    return lax.dot_general(a, b, (((0,), (0,)), ((), ())), preferred_element_type=F32)


def iota(shape, dim):
    return lax.broadcasted_iota(jnp.int32, shape, dim)


def call(kernel, out_shape, n_in, flops=0, n_bytes=0, name=None):
    vmem = pl.BlockSpec(memory_space=pltpu.VMEM)
    return pl.pallas_call(
        kernel,
        out_shape=out_shape,
        in_specs=[pl.BlockSpec(memory_space=pltpu.SMEM)] + [vmem] * n_in,
        out_specs=jax.tree.map(lambda _: vmem, out_shape),
        compiler_params=pltpu.CompilerParams(vmem_limit_bytes=VMEM_LIMIT),
        cost_estimate=pl.CostEstimate(flops=flops, bytes_accessed=n_bytes, transcendentals=0),
        name=name,
    )


def row_of(column, width):
    n = column.shape[0]
    shape = (n, width)
    return jnp.sum(jnp.where(iota(shape, 0) == iota(shape, 1), column, 0.0), axis=0, keepdims=True)


def column_of(row, n):
    shape = (n, row.shape[1])
    return jnp.sum(jnp.where(iota(shape, 0) == iota(shape, 1), row, 0.0), axis=1, keepdims=True)


def rows_block(rows):
    block = jnp.zeros((META, LANES), F32)
    which = iota((META, LANES), 0)
    for index, row in enumerate(rows):
        block = jnp.where(which == index, row, block)
    return block


def hi_lo(rows):
    hi = [row.astype(BF).astype(F32) for row in rows]
    lo = [row - top for row, top in zip(rows, hi)]
    return rows_block(hi + lo).astype(BF)


def from_hi_lo(block, count):
    block = block.astype(F32)
    return [block[i : i + 1] + block[count + i : count + i + 1] for i in range(count)]


def dispatch_kernel(ids, tok_a, tok_b, grad_a, grad_b, meta_a, meta_b, *outs, cap, chips):
    match_out, sends = outs[0], outs[1:]
    ep = ids[0]
    tok_rows = tok_a.shape[0]
    both = CORES * tok_rows
    rows = CORES * cap
    meta = jnp.concatenate([jnp.transpose(meta_a[...])[:META], jnp.transpose(meta_b[...])[:META]], axis=1)
    expert = (iota((chips, both), 0) * CORES) ^ ep
    first = meta[0:1].astype(jnp.int32) == expert
    second = meta[1:2].astype(jnp.int32) == expert
    named = jnp.where(first | second, 1.0, 0.0)
    weight = jnp.where(first, meta[2:3], 0.0) + jnp.where(second, meta[3:4], 0.0)
    i0, i1 = iota((both, both), 0), iota((both, both), 1)
    before = (i0 < i1) & ((i0 >= tok_rows) == (i1 >= tok_rows))
    rank = nn(named.astype(BF), jnp.where(before, 1.0, 0.0).astype(BF)).astype(jnp.int32)
    lane = iota((chips, both), 1)
    slot = jnp.where(first | second, rank + jnp.where(lane >= tok_rows, cap, 0), -1)
    tok = jnp.concatenate([tok_a[...], tok_b[...]], axis=0)
    grad = jnp.concatenate([grad_a[...], grad_b[...]], axis=0)
    for k in range(chips):
        hit = slot[k : k + 1] == iota((LANES, both), 0)
        match = jnp.where(hit, 1.0, 0.0)
        match_out[k * LANES : (k + 1) * LANES, :] = match.astype(BF)
        match_b = match[:rows].astype(BF)
        sends[k][0:rows, :] = nn(match_b, tok).astype(BF)
        sends[k][rows : 2 * rows, :] = nn(match_b, grad).astype(BF)
        scale = jnp.sum(jnp.where(hit, weight[k : k + 1], 0.0), axis=1, keepdims=True)
        sends[k][2 * rows : 2 * rows + META, 0:LANES] = jnp.broadcast_to(
            row_of(scale, LANES), (META, LANES)
        ).astype(BF)


def expert_kernel(ids, *refs, streams, parts, group, rows, first_sizes):
    n_parts = len(parts)
    pieces = [refs[s * n_parts : (s + 1) * n_parts] for s in range(streams)]
    at = streams * n_parts
    scales = refs[at : at + streams]
    gate, up, down = refs[at + streams : at + streams + 3]
    outs = refs[at + streams + 3 :]
    tp = ids[1]
    hidden_units = gate.shape[0]
    width = pieces[0][0].shape[1]
    srows = group * rows
    total = streams * srows

    def columns(offset):
        return pl.ds(pl.multiple_of((tp ^ offset) * width, width), width)

    pre_gate = jnp.zeros((total, hidden_units), F32)
    pre_up = jnp.zeros((total, hidden_units), F32)
    back = jnp.zeros((total, hidden_units), F32)
    for j in range(n_parts):
        tok = jnp.concatenate([pieces[s][j][0:srows, :] for s in range(streams)], axis=0)
        grad = jnp.concatenate([pieces[s][j][srows : 2 * srows, :] for s in range(streams)], axis=0)
        cols = columns(j)
        pre_gate += nt(tok, gate[:, cols])
        pre_up += nt(tok, up[:, cols])
        back += nt(grad, down[:, cols])
    scale = jnp.concatenate(
        [
            column_of(scales[s][kk : kk + 1, 0:LANES].astype(F32), rows)
            for s in range(streams)
            for kk in range(group)
        ],
        axis=0,
    )
    squash = jax.nn.sigmoid(pre_gate)
    activated = pre_gate * squash
    hidden = (activated * pre_up).astype(BF).astype(F32)
    products = jnp.sum(hidden * back, axis=1, keepdims=True)
    hidden_grad = scale * back
    gate_delta = (hidden_grad * pre_up * squash * (1.0 + pre_gate * (1.0 - squash))).astype(BF)
    up_delta = (hidden_grad * activated).astype(BF)
    outs[0][...] = gate_delta
    outs[1][...] = up_delta
    outs[2][...] = (scale * hidden).astype(BF)
    outs = outs[3:]
    for s in range(streams):
        mine = [
            row_of(products[s * srows + kk * rows : s * srows + (kk + 1) * rows], LANES) for kk in range(group)
        ]
        outs[0 + s * 2 + sum(first_sizes[:s]) - s + 1][...] = rows_block(mine)
    bases = [s * 2 + sum(first_sizes[:s]) - s for s in range(streams)]
    for j in range(n_parts):
        cols = columns(j)
        part = (nn(gate_delta, gate[:, cols]) + nn(up_delta, up[:, cols])).astype(BF)
        for s in range(streams):
            ja, jb = parts[j][s]
            target = outs[bases[s]] if ja == 0 else outs[bases[s] + 1 + ja]
            target[jb * srows : (jb + 1) * srows, :] = part[s * srows : (s + 1) * srows]
    for s in range(streams):
        mine = [
            row_of(products[s * srows + kk * rows : s * srows + (kk + 1) * rows], LANES) for kk in range(group)
        ]
        second = n_parts // first_sizes[s]
        for ja in range(1, first_sizes[s]):
            outs[bases[s] + 1 + ja][second * srows : second * srows + META, 0:LANES] = hi_lo(mine)


def add_kernel(ids, *refs, peers, group, srows, second, last):
    kept, kept_products = refs[0], refs[1]
    got = refs[2 : 2 + peers]
    outs = refs[2 + peers :]
    products = [kept_products[kk : kk + 1, :] for kk in range(group)]
    for message in got:
        theirs = from_hi_lo(message[second * srows : second * srows + META, 0:LANES], group)
        products = [a + b for a, b in zip(products, theirs)]

    def total(jb):
        value = kept[jb * srows : (jb + 1) * srows, :].astype(F32)
        for message in got:
            value = value + message[jb * srows : (jb + 1) * srows, :].astype(F32)
        return value.astype(BF)

    if last:
        outs[0][0:srows, :] = total(0)
        outs[0][srows : srows + META, 0:LANES] = hi_lo(products)
        return
    outs[0][...] = total(0)
    outs[1][...] = rows_block(products)
    for jb in range(1, second):
        outs[1 + jb][0:srows, :] = total(jb)
        outs[1 + jb][srows : srows + META, 0:LANES] = hi_lo(products)


def weight_kernel(ids, *refs, streams, n_parts, srows, start, chunks):
    pieces = [refs[s * n_parts : (s + 1) * n_parts] for s in range(streams)]
    deltas = refs[streams * n_parts : streams * n_parts + chunks]
    out = refs[streams * n_parts + chunks]
    width = pieces[0][0].shape[1]
    delta = jnp.concatenate([d[...] for d in deltas], axis=0)
    for j in range(n_parts):
        rows = jnp.concatenate([pieces[s][j][start : start + srows, :] for s in range(streams)], axis=0)
        cols = pl.ds(pl.multiple_of((ids[1] ^ j) * width, width), width)
        out[:, cols] = tn(delta, rows).astype(BF)


def combine_kernel(ids, match, meta_a, meta_b, *refs, chips, group, rows):
    returned = refs[:chips]
    own_rows, own_products, message = refs[chips:]
    tok_rows = meta_a.shape[0]
    both = CORES * tok_rows
    meta = jnp.concatenate([jnp.transpose(meta_a[...])[:META], jnp.transpose(meta_b[...])[:META]], axis=1)
    value = jnp.zeros((both, own_rows.shape[1]), F32)
    sums = [jnp.zeros((1, both), F32) for _ in range(2)]
    picks = jnp.concatenate([match[k * LANES : k * LANES + rows, :] for k in range(chips)], axis=0)
    landed = jnp.concatenate([returned[k][0:rows, :] for k in range(chips)], axis=0)
    value = tn(picks, landed)
    for k in range(chips):
        expert = ids[0] ^ (k * CORES)
        block = returned[k][rows : rows + META, 0:LANES]
        found = nn(block, match[k * LANES : (k + 1) * LANES, :])
        kk = k % group
        mine = found[kk : kk + 1] + found[group + kk : group + kk + 1]
        for choice in range(2):
            chosen = meta[choice : choice + 1].astype(jnp.int32) == expert
            sums[choice] = sums[choice] + jnp.where(chosen, mine, 0.0)
    own_rows[...] = value[:tok_rows]
    own_products[...] = rows_block([s[:, :tok_rows] for s in sums])
    message[0:tok_rows, :] = value[tok_rows:].astype(BF)
    message[tok_rows : tok_rows + META, 0:LANES] = hi_lo([s[:, tok_rows:] for s in sums])


def finish_kernel(ids, own_rows, own_products, message, token_grad, weight_grad):
    tok_rows = own_rows.shape[0]
    token_grad[...] = (own_rows[...] + message[0:tok_rows, :].astype(F32)).astype(BF)
    theirs = from_hi_lo(message[tok_rows : tok_rows + META, 0:LANES], 2)
    columns = [column_of(own_products[i : i + 1, :] + theirs[i], tok_rows) for i in range(2)]
    weight_grad[...] = jnp.concatenate(columns, axis=1)


def local(tokens, out_grad, routes, route_weights, gate_proj, up_proj, down_proj, shared_hidden):
    ep_count = lax.axis_size("ep")
    tp_count = lax.axis_size("tp")
    chips = ep_count // CORES
    tok_rows, per_token = routes.shape
    width = tokens.shape[1]
    num_experts = gate_proj.shape[0] * ep_count
    hidden_units, features = gate_proj.shape[1:]
    capacity = max(2, 5 * tok_rows * per_token // (4 * num_experts))
    cap = -(-capacity // 8) * 8
    rows = CORES * cap
    streams = min(chips, 4)
    group = chips // streams
    srows = group * rows
    tx = 1 << ((tp_count.bit_length() - 1) // 2)
    ty = tp_count // tx
    sds = jax.ShapeDtypeStruct
    gate, up, down = gate_proj[0], up_proj[0], down_proj[0]

    ep_index = lax.axis_index("ep")
    ids = jnp.stack([ep_index, lax.axis_index("tp")]).astype(jnp.int32)
    meta = jnp.concatenate(
        [
            routes.astype(F32),
            route_weights.astype(BF).astype(F32),
            jnp.zeros((tok_rows, LANES - 2 * per_token), F32),
        ],
        axis=1,
    )
    meta_b = xor_permute(meta, "ep", 1)
    tok_b = xor_permute(tokens, "ep", 1)
    grad_b = xor_permute(out_grad, "ep", 1)
    hid_b = xor_permute(shared_hidden, "ep", 1)

    message = sds((2 * rows + META, width), BF)
    outs = call(
        functools.partial(dispatch_kernel, cap=cap, chips=chips),
        [sds((chips * LANES, CORES * tok_rows), BF)] + [message] * chips,
        6,
        flops=4 * chips * rows * 2 * tok_rows * width,
        n_bytes=4 * chips * rows * width * 2,
        name="dispatch",
    )(ids, tokens, tok_b, out_grad, grad_b, meta, meta_b)
    match, sends = outs[0], outs[1:]

    landed = [sends[0]] + [xor_permute(sends[k], "ep", k * CORES) for k in range(1, chips)]

    def first_axis(s):
        return (tx, 1, ty, tx) if s % 2 == 0 else (ty, tx, tx, 1)

    blocks, scales = [], []
    for s in range(streams):
        mine = landed[s * group : (s + 1) * group]
        if group == 1:
            block = mine[0][0 : 2 * rows]
            scale = mine[0][2 * rows :]
        else:
            block = jnp.concatenate([m[0:rows] for m in mine] + [m[rows : 2 * rows] for m in mine], axis=0)
            scale = jnp.concatenate([m[2 * rows : 2 * rows + 1] for m in mine], axis=0)
            scale = jnp.pad(scale, ((0, META - group), (0, 0)))
        blocks.append(block)
        scales.append(scale)
    pieces = []
    for s in range(streams):
        n_first, step_first, n_second, step_second = first_axis(s)
        line = [blocks[s]] + [xor_permute(blocks[s], "tp", ja * step_first) for ja in range(1, n_first)]
        got = {}
        for ja in range(n_first):
            got[ja * step_first] = line[ja]
            for jb in range(1, n_second):
                got[ja * step_first + jb * step_second] = xor_permute(line[ja], "tp", jb * step_second)
        pieces.append([got[j] for j in range(tp_count)])

    def place(j, s):
        n_first, step_first, n_second, step_second = first_axis(s)
        return (j // step_first) % n_first, (j // step_second) % n_second

    chunk_streams = [list(range(streams))[i : i + 2] for i in range(0, streams, 2)]
    deltas = []
    finals = [None] * streams
    for chunk in chunk_streams:
        n = len(chunk)
        total = n * srows
        delta = sds((total, hidden_units), BF)
        out_shape = [delta] * 3
        for s in chunk:
            n_first, _, n_second, _ = first_axis(s)
            out_shape += [sds((n_second * srows, width), BF), sds((META, LANES), F32)]
            out_shape += [sds((n_second * srows + META, width), BF)] * (n_first - 1)
        outs = call(
            functools.partial(
                expert_kernel,
                streams=n,
                parts=[[place(j, s) for s in chunk] for j in range(tp_count)],
                group=group,
                rows=rows,
                first_sizes=[first_axis(s)[0] for s in chunk],
            ),
            out_shape,
            n * tp_count + n + 3,
            flops=10 * total * hidden_units * features,
            n_bytes=3 * hidden_units * features * 2,
            name="expert",
        )(ids, *[v for s in chunk for v in pieces[s]], *[scales[s] for s in chunk], gate, up, down)
        deltas.append(outs[:3])
        outs = outs[3:]
        for s in chunk:
            n_first, step_first, n_second, step_second = first_axis(s)
            kept, kept_products = outs[0], outs[1]
            got = [xor_permute(outs[1 + ja], "tp", ja * step_first) for ja in range(1, n_first)]
            outs = outs[1 + n_first :]
            mids = call(
                functools.partial(
                    add_kernel, peers=len(got), group=group, srows=srows, second=n_second, last=False
                ),
                [sds((srows, width), BF), sds((META, LANES), F32)]
                + [sds((srows + META, width), BF)] * (n_second - 1),
                2 + len(got),
                name="add_first",
            )(ids, kept, kept_products, *got)
            got = [xor_permute(mids[1 + jb], "tp", jb * step_second) for jb in range(1, n_second)]
            finals[s] = call(
                functools.partial(add_kernel, peers=len(got), group=group, srows=srows, second=1, last=True),
                [sds((srows + META, width), BF)],
                2 + len(got),
                name="add_last",
            )(ids, mids[0], mids[1], *got)[0]

    returned = []
    for k in range(chips):
        value = finals[k // group]
        if group > 1:
            kk = k % group
            value = jnp.concatenate([value[kk * rows : (kk + 1) * rows], value[srows:]], axis=0)
        returned.append(value if k == 0 else xor_permute(value, "ep", k * CORES))
    own_rows, own_products, to_partner = call(
        functools.partial(combine_kernel, chips=chips, group=group, rows=rows),
        [sds((tok_rows, width), F32), sds((META, LANES), F32), sds((tok_rows + META, width), BF)],
        3 + chips,
        name="combine",
    )(ids, match, meta, meta_b, *returned)
    from_partner = xor_permute(to_partner, "ep", 1)
    token_grad, weight_grad = call(
        finish_kernel,
        [sds((tok_rows, width), BF), sds((tok_rows, per_token), F32)],
        3,
        name="finish",
    )(ids, own_rows, own_products, from_partner)

    grads = []
    for which in range(3):
        grads.append(
            call(
                functools.partial(
                    weight_kernel,
                    streams=streams,
                    n_parts=tp_count,
                    srows=srows,
                    start=srows if which == 2 else 0,
                    chunks=len(deltas),
                ),
                [sds((hidden_units, features), BF)],
                streams * tp_count + len(deltas),
                flops=2 * streams * srows * hidden_units * features,
                n_bytes=hidden_units * features * 2,
                name="weight_grad",
            )(ids, *[v for s in range(streams) for v in pieces[s]], *[d[which] for d in deltas])[0][None]
        )
    gate_grad, up_grad, down_grad = grads

    slice_rows = shared_hidden.shape[1] // ep_count
    hid = jnp.concatenate([shared_hidden, hid_b], axis=0)
    grad = jnp.concatenate([out_grad, grad_b], axis=0)
    shared = None
    for k in range(chips):
        cut = lax.dynamic_slice_in_dim(hid, (ep_index ^ (k * CORES)) * slice_rows, slice_rows, axis=1)
        part = tn(cut, grad)
        if k == 0:
            shared = part
        else:
            shared = shared + xor_permute(part.astype(BF), "ep", k * CORES).astype(F32)
    return (token_grad, weight_grad, gate_grad, up_grad, down_grad, shared)


def solution(mesh):
    return jax.shard_map(
        local,
        mesh=mesh,
        in_specs=(
            P("ep", "tp"),
            P("ep", "tp"),
            P("ep", None),
            P("ep", None),
            P("ep", "tp", None),
            P("ep", "tp", None),
            P("ep", "tp", None),
            P("ep", None),
        ),
        out_specs=(
            P("ep", "tp"),
            P("ep", None),
            P("ep", "tp", None),
            P("ep", "tp", None),
            P("ep", "tp", None),
            P("ep", "tp"),
        ),
        check_vma=False,
    )
```
